32 devices in a mesh: sp: 8 (over z, x), tp: 4 (over y, core).
Axes of the slice: x: 2, y: 2, z: 4, core: 2. Of those that a mesh axis runs over, the one named last changes fastest.
Arguments:
- residual_signal: bfloat16 [1024, 2048], P('sp', 'tp'), may hold values from -90 to 90
- lifted_signal: bfloat16 [1024, 1024], P('sp', 'tp'), may hold values from -6 to 6
- discrete_timestep: float32 [64, 1024], P('tp', 'sp'), may hold values from 0.17 to 4.2
- additional_log_fading: float32 [64, 1024], P('tp', 'sp'), may hold values from -2.1 to 0
- paired_fading: float32 [2, 32, 64], replicated, may hold values from 1.953125e-05 to 0.0625
- unpaired_fading: float32 [2, 32, 32], replicated, may hold values from 1.953125e-05 to 0.0625
- paired_twist: float32 [2, 32, 64], replicated, may hold values from -3.140625 to 3.140625
- unpaired_twist: float32 [2, 32, 32], replicated, may hold values from -3.140625 to 3.140625
- paired_latent_linears: float32 [2, 2, 2, 32, 64, 16], replicated, may hold values from -1 to 1
- unpaired_latent_linears: float32 [2, 2, 2, 32, 32, 16], replicated, may hold values from -1 to 1
- skip_coefficient: float32 [1024], replicated, may hold values from -4 to 4
- closing_norm_multiplier: float32 [1024], replicated, may hold values from 0.1 to 1.9
- emitted_linear: bfloat16 [1024, 2048], replicated, may hold values from -0.1875 to 0.1875
- leading_norm_multiplier: float32 [2048], replicated, may hold values from 0.1 to 1.9
- raising_linear: bfloat16 [2048, 8192], P('sp', 'tp'), may hold values from -0.125 to 0.125
- lowering_linear: bfloat16 [8192, 2048], P('tp', 'sp'), may hold values from -0.0625 to 0.0625
Outputs:
- layer_out: bfloat16 [1024, 2048], P('sp', 'tp')
The draws below stay inside these ranges and needn't reach their ends.
All inputs are finite; a program needn't handle non-finite values.
Results may differ from the reference program's by a relative error of at most 0.008.
Values may be sent and summed in bfloat16 or wider, within the bound.
No kernel may reach another device: no remote copies, remote signals or barrier semaphores. Data moves between devices by JAX's collectives and lax.ppermute only.
A program may use at most 128 MiB of HBM per device.

```python
import math
import jax
import jax.numpy as jnp
from jax import lax

D = 2048
FF = 8192
MIXER_BANDS = 64
CHAN = 16
STATE_LONG = 64
STATE_SHORT = 32
NORM_W = 128
TOK_DEV = 128
SSM_W = 1024
TOKENS = 1024
N_TP = 4


def draw_residual_signal(key, part):
    keys = jax.random.split(jax.random.fold_in(key, 5), 3)
    column = 0.4 * 10.0 ** (jnp.arange(D, dtype=jnp.float32) / D)
    column = column * jax.random.uniform(keys[0], (D,), jnp.float32, 0.7, 1.4)
    base = jnp.clip(jax.random.normal(keys[1], (TOKENS, D), jnp.float32), -4.0, 4.0)
    row_scale = jnp.exp(jax.random.uniform(keys[2], (TOKENS,), jnp.float32, math.log(0.5), math.log(4.0)))
    return (base * row_scale[:, None] * column[None, :]).astype(jnp.bfloat16)


def draw_discrete_timestep(key, part):
    keys = jax.random.split(jax.random.fold_in(key, 7), 2)
    span = TOK_DEV // 2
    count = TOKENS // span
    lowest, highest, rough_low, rough_high = (0.5, 2.0, 0.5, 1.5)
    factor = jnp.exp(jax.random.uniform(keys[0], (count,), jnp.float32, math.log(lowest), math.log(highest)))
    along = jnp.repeat(factor, span)
    rough = jax.random.uniform(keys[1], (MIXER_BANDS, TOKENS), jnp.float32, rough_low, rough_high)
    return along[None, :] * rough


def draw_additional_log_fading(key, part):
    keys = jax.random.split(jax.random.fold_in(key, 9), 2)
    places = jax.random.randint(keys[0], (MIXER_BANDS, 3), 0, TOKENS)
    values = jax.random.uniform(keys[1], (MIXER_BANDS, 3), jnp.float32, math.log(0.5), math.log(0.8))
    hits = (jnp.arange(TOKENS)[None, None, :] == places[:, :, None]).astype(jnp.float32)
    return jnp.sum(hits * values[:, :, None], axis=1)


def draw_rates(key, states):
    keys = jax.random.split(key, 4)
    share = 8
    quick = jax.random.randint(keys[0], (2, MIXER_BANDS // 2), 0, 16) < share
    quick_rate = jnp.exp(jax.random.uniform(keys[1], (2, MIXER_BANDS // 2), jnp.float32, math.log(0.01), math.log(0.025)))
    slow_rate = jnp.exp(jax.random.uniform(keys[2], (2, MIXER_BANDS // 2), jnp.float32, math.log(0.02), math.log(0.12))) / TOKENS
    base = jnp.where(quick, quick_rate, slow_rate)
    spread = jnp.exp(jax.random.uniform(keys[3], (2, MIXER_BANDS // 2, states), jnp.float32, 0.0, math.log(2.5)))
    return base[:, :, None] * spread


def draw_paired_fading(key, part):
    return draw_rates(jax.random.fold_in(key, 11), STATE_LONG)


def draw_unpaired_fading(key, part):
    return draw_rates(jax.random.fold_in(key, 12), STATE_SHORT)


def level_of(key, dims, cuts, least, high):
    def one(axis_at, parts):
        heights = jax.random.uniform(jax.random.fold_in(jax.random.fold_in(key, 6), axis_at), (parts,), jnp.float32, least / len(cuts), high / len(cuts))
        return jnp.repeat(jnp.exp(heights), dims[axis_at] // parts).reshape((-1,) + (1,) * (len(dims) - axis_at - 1))

    level = one(*cuts[0])
    for cut in cuts[1:]:
        level = level * one(*cut)
    return level


def scatter_about(stream_key, shape, deviation, most, cuts=(), kind=jnp.bfloat16):
    drawn = jax.random.normal(stream_key, shape, jnp.float32) * deviation
    if len(cuts) > 0:
        drawn = level_of(stream_key, shape, cuts, -0.22, 0.18) * drawn
    return jnp.clip(drawn, min=-most, max=most).astype(kind)


def setup_inputs(seed: int = 0) -> dict:
    seeds = jax.random.split(jax.random.key(seed), 17)
    residual_signal = draw_residual_signal(jax.random.fold_in(seeds[16], 71), 0)
    lifted_signal = scatter_about(seeds[1], (TOKENS, SSM_W), 1.0, 6.0, ((0, 8), (1, 4)))
    discrete_timestep = draw_discrete_timestep(jax.random.fold_in(seeds[16], 71), 0)
    additional_log_fading = draw_additional_log_fading(jax.random.fold_in(seeds[16], 71), 0)
    paired_fading = draw_paired_fading(jax.random.fold_in(seeds[16], 71), 0)
    unpaired_fading = draw_unpaired_fading(jax.random.fold_in(seeds[16], 71), 0)
    paired_twist = jnp.clip(jax.random.uniform(seeds[6], (2, MIXER_BANDS // 2, STATE_LONG), jnp.float32, -3.140625, 3.140625), -3.140625, 3.140625)
    unpaired_twist = jnp.clip(jax.random.uniform(seeds[7], (2, MIXER_BANDS // 2, STATE_SHORT), jnp.float32, -3.140625, 3.140625), -3.140625, 3.140625)
    paired_latent_linears = scatter_about(seeds[8], (2, 2, 2, MIXER_BANDS // 2, STATE_LONG, CHAN), (2 * CHAN) ** -0.5, 1.0, (), jnp.float32)
    unpaired_latent_linears = scatter_about(seeds[9], (2, 2, 2, MIXER_BANDS // 2, STATE_SHORT, CHAN), (2 * CHAN) ** -0.5, 1.0, (), jnp.float32)
    skip_coefficient = scatter_about(seeds[10], (SSM_W,), 1.0, 4.0, (), jnp.float32)
    closing_norm_multiplier = jnp.clip(1.0 + 0.18 * jax.random.normal(seeds[11], (SSM_W,), jnp.float32), 0.1, 1.9)
    emitted_linear = scatter_about(seeds[12], (SSM_W, D), SSM_W ** -0.5, 0.1875)
    leading_norm_multiplier = jnp.clip(1.0 + 0.18 * jax.random.normal(seeds[13], (D,), jnp.float32), 0.1, 1.9)
    raising_linear = scatter_about(seeds[14], (D, FF), D ** -0.5, 0.125, ((0, 8), (1, 4)))
    lowering_linear = scatter_about(seeds[15], (FF, D), FF ** -0.5, 0.0625, ((0, 4), (1, 8)))
    return {"residual_signal": residual_signal, "lifted_signal": lifted_signal, "discrete_timestep": discrete_timestep, "additional_log_fading": additional_log_fading, "paired_fading": paired_fading, "unpaired_fading": unpaired_fading, "paired_twist": paired_twist, "unpaired_twist": unpaired_twist, "paired_latent_linears": paired_latent_linears, "unpaired_latent_linears": unpaired_latent_linears, "skip_coefficient": skip_coefficient, "closing_norm_multiplier": closing_norm_multiplier, "emitted_linear": emitted_linear, "leading_norm_multiplier": leading_norm_multiplier, "raising_linear": raising_linear, "lowering_linear": lowering_linear}


EPSILON = 1e-06

def combine_maps(early, later):
    first_re, first_im, base_re, base_im = early
    next_re, next_im, add_re, add_im = later
    return (next_re * first_re - next_im * first_im, next_re * first_im + next_im * first_re, next_re * base_re - next_im * base_im + add_re, next_re * base_im + next_im * base_re + add_im)

def step_maps(group_inputs, pace, surge_entries, decay_rate, turn_rate, input_re, input_im):
    scaled = pace[:, :, None]
    magnitude = jnp.exp(-decay_rate[None] * scaled + surge_entries[:, :, None])
    angle = turn_rate[None] * scaled
    weight_in = jnp.sqrt(-jnp.expm1(-2.0 * decay_rate[None] * scaled))
    drive_re = jnp.einsum('ngj,gpj->ngp', group_inputs, input_re, precision=lax.Precision.HIGHEST) * weight_in
    drive_im = jnp.einsum('ngj,gpj->ngp', group_inputs, input_im, precision=lax.Precision.HIGHEST) * weight_in
    return (magnitude * jnp.cos(angle), magnitude * jnp.sin(angle), drive_re, drive_im)

def readout(state_re, state_im, read_re, read_im):
    return jnp.einsum('ngp,gpj->ngj', state_re, read_re, precision=lax.Precision.HIGHEST) - jnp.einsum('ngp,gpj->ngj', state_im, read_im, precision=lax.Precision.HIGHEST)

def kind_output(group_inputs, pace, surge_entries, decay_rate, turn_rate, projection):
    batch_number = group_inputs.shape[0]
    count = batch_number // TOK_DEV
    width = group_inputs.shape[1]
    states = decay_rate.shape[-1]
    input_blocks = group_inputs.reshape(count, TOK_DEV, width, CHAN)
    pace_blocks = pace.reshape(count, TOK_DEV, width)
    jolt_blocks = surge_entries.reshape(count, TOK_DEV, width)
    result = jnp.zeros((count, TOK_DEV, width, CHAN), jnp.float32)
    for direction in range(2):
        backward = direction == 1
        edge = 0 if backward else -1

        def each_block(carry, pieces, direction=direction, backward=backward, edge=edge):
            block_inputs, block_pace, block_jolts = pieces
            maps = step_maps(block_inputs, block_pace, block_jolts, decay_rate[direction], turn_rate[direction], projection[direction, 0, 0], projection[direction, 0, 1])
            prefix_re, prefix_im, state_re, state_im = lax.associative_scan(combine_maps, maps, reverse=backward, axis=0)
            carry_re, carry_im = carry
            state_re = state_re + prefix_re * carry_re[None] - prefix_im * carry_im[None]
            state_im = state_im + prefix_re * carry_im[None] + prefix_im * carry_re[None]
            values = readout(state_re, state_im, projection[direction, 1, 0], projection[direction, 1, 1])
            return ((state_re[edge], state_im[edge]), values)
        start = (jnp.zeros((width, states), jnp.float32), jnp.zeros((width, states), jnp.float32))
        _, values = lax.scan(each_block, start, (input_blocks, pace_blocks, jolt_blocks), reverse=backward)
        result = result + values
    return result.reshape(batch_number, width, CHAN)

def reference(residual_signal, lifted_signal, discrete_timestep, additional_log_fading, paired_fading, unpaired_fading, paired_twist, unpaired_twist, paired_latent_linears, unpaired_latent_linears, skip_coefficient, closing_norm_multiplier, emitted_linear, leading_norm_multiplier, raising_linear, lowering_linear):
    batch_number = residual_signal.shape[0]
    grouped = lifted_signal.astype(jnp.float32).reshape(batch_number, MIXER_BANDS // 2, 2, CHAN)
    pace = discrete_timestep.T.reshape(batch_number, MIXER_BANDS // 2, 2)
    surge_entries = additional_log_fading.T.reshape(batch_number, MIXER_BANDS // 2, 2)
    long_out = kind_output(grouped[:, :, 0], pace[:, :, 0], surge_entries[:, :, 0], paired_fading, paired_twist, paired_latent_linears)
    short_out = kind_output(grouped[:, :, 1], pace[:, :, 1], surge_entries[:, :, 1], unpaired_fading, unpaired_twist, unpaired_latent_linears)
    ssm_out = jnp.stack([long_out, short_out], axis=2).reshape(batch_number, SSM_W)
    activated = jax.nn.gelu(ssm_out + skip_coefficient[None] * grouped.reshape(batch_number, SSM_W))
    heads = activated.reshape(batch_number, SSM_W // NORM_W, NORM_W)
    heads = heads * lax.rsqrt(lax.optimization_barrier(jnp.mean(heads * heads, axis=2, keepdims=True)) + EPSILON)
    combined_result = (heads.reshape(batch_number, SSM_W) * closing_norm_multiplier[None]).astype(jnp.bfloat16)
    inner_activity = residual_signal.astype(jnp.float32) + jnp.dot(combined_result, emitted_linear, preferred_element_type=jnp.float32)
    scale = lax.rsqrt(lax.optimization_barrier(jnp.mean(inner_activity * inner_activity, axis=1, keepdims=True)) + EPSILON)
    normed = (inner_activity * scale * leading_norm_multiplier[None]).astype(jnp.bfloat16)
    block_width = FF // N_TP
    feed = jnp.zeros((batch_number, D), jnp.float32)
    for member in range(N_TP):
        upward = jnp.dot(normed, raising_linear[:, member * block_width:(member + 1) * block_width], preferred_element_type=jnp.float32)
        hidden = jnp.square(jax.nn.relu(upward)).astype(jnp.bfloat16)
        product = jnp.dot(hidden, lowering_linear[member * block_width:(member + 1) * block_width], preferred_element_type=jnp.float32).astype(jnp.bfloat16)
        feed = feed + product.astype(jnp.float32)
    return (inner_activity + feed).astype(jnp.bfloat16)
```

```python
import jax
import jax.numpy as jnp
from jax import lax
from jax.experimental import pallas as pl
from jax.experimental.pallas import tpu as pltpu
from jax.sharding import Mesh
from jax.sharding import PartitionSpec as P

CHAN = 16
NORM_W = 128
CHUNKS = 8
LANES = 128
EPSILON = 1e-06
HALVES = 2
SIN = (3.1415926532428884, -5.167712741152494, 2.5501627931734125, -0.5992473907509345, 0.08203117351788075, -0.00700041798679132)
COS = (0.9999999997799042, -4.934802137078826, 4.058709159556303, -1.33521200305024, 0.23493731381503577, -0.02439632434807213)
FADE = (1.0, -1.0 / 2, 1.0 / 6, -1.0 / 24, 1.0 / 120, -1.0 / 720, 1.0 / 5040, -1.0 / 40320)
F32 = jnp.float32
BF16 = jnp.bfloat16


def horner(coefficients, x):
    total = jnp.full_like(x, coefficients[-1])
    for c in coefficients[-2::-1]:
        total = total * x + c
    return total


def sin_cos(angle):
    halves = angle * 0.3183098861837907
    whole = jnp.round(halves)
    r = halves - whole
    z = r * r
    odd = whole * 0.5
    odd = odd - jnp.floor(odd)
    sign = 1.0 - 4.0 * odd
    return sign * r * horner(SIN, z), sign * horner(COS, z)


def one_minus_exp(z):
    return jnp.where(z < 0.5, z * horner(FADE, z), 1.0 - jnp.exp(-z))


def iota(shape, axis):
    return lax.broadcasted_iota(jnp.int32, shape, axis)


def time_of_row(row, tokens, backward):
    steps = tokens // CHUNKS
    t = (row % CHUNKS) * steps + row // CHUNKS
    return tokens - 1 - t if backward else t


def group_of_lane(lane, pairs, long_states, short_states):
    border = pairs * long_states
    return jnp.where(
        lane < border,
        2 * (lane // long_states),
        2 * ((lane - border) // short_states) + 1,
    )


def tiled(part, copies):
    return jnp.concatenate([part] * copies, axis=-1) if copies > 1 else part


def spread(long_part, short_part):
    pairs, chan, long_states = long_part.shape
    short_states = short_part.shape[2]
    rows = pairs * 2 * chan
    long_rows = jnp.concatenate([long_part, jnp.zeros_like(long_part)], axis=1)
    short_rows = jnp.concatenate([jnp.zeros_like(short_part), short_part], axis=1)
    halves = []
    for part, states in ((long_rows, long_states), (short_rows, short_states)):
        part = part.reshape(rows, states)
        part = tiled(part, LANES // states)
        part = tiled(part, pairs * states // LANES)
        keep = iota(part.shape, 1) // states == iota(part.shape, 0) // (2 * chan)
        halves.append(jnp.where(keep, part, 0.0))
    return jnp.concatenate(halves, axis=1).astype(BF16)


def flat_row(long_part, short_part):
    halves = []
    for part in (long_part, short_part):
        pairs, states = part.shape
        wide = tiled(tiled(part, LANES // states), pairs * states // LANES)
        keep = iota(wide.shape, 1) // states == iota(wide.shape, 0)
        halves.append(jnp.sum(jnp.where(keep, wide, 0.0), axis=0, keepdims=True))
    return jnp.concatenate(halves, axis=1)


def three_parts(x):
    high = x.astype(BF16).astype(F32)
    rest = x - high
    middle = rest.astype(BF16).astype(F32)
    return [high, middle, rest - middle]


def scan_kernel(
    rank_ref, input_ref, pace_ref, surge_ref, long_rate_ref, short_rate_ref, long_turn_ref, short_turn_ref,
    long_maps_ref, short_maps_ref, maps_ref, ends_ref, tail_ref,
):
    tokens, width = input_ref.shape
    groups = pace_ref.shape[0]
    _, pairs, long_states = long_rate_ref.shape
    short_states = short_rate_ref.shape[2]
    lanes = pairs * (long_states + short_states)
    steps = tokens // CHUNKS
    pieces = three_parts(pace_ref[...]) + three_parts(surge_ref[...])
    six = jnp.concatenate(pieces, axis=0).astype(BF16)
    inputs = input_ref[...]
    row = iota((6 * groups, lanes), 0)
    owner = group_of_lane(iota((6 * groups, lanes), 1), pairs, long_states, short_states)
    match = row % groups == owner
    pace_map = jnp.where(match & (row < 3 * groups), 1.0, 0.0).astype(BF16)
    surge_map = jnp.where(match & (row >= 3 * groups), 1.0, 0.0).astype(BF16)
    for d in range(2):
        place = time_of_row(iota((tokens, tokens), 0), tokens, d == 1) == iota((tokens, tokens), 1)
        place = jnp.where(place, 1.0, 0.0).astype(BF16)
        ordered = jnp.dot(place, inputs, preferred_element_type=F32).astype(BF16)
        six_rows = lax.dot_general(
            place, six, (((1,), (1,)), ((), ())), preferred_element_type=F32
        ).astype(BF16)
        rate = flat_row(long_rate_ref[d], short_rate_ref[d])
        turn = flat_row(long_turn_ref[d], short_turn_ref[d])
        in_re = spread(long_maps_ref[d, 0, 0], short_maps_ref[d, 0, 0])
        in_im = spread(long_maps_ref[d, 0, 1], short_maps_ref[d, 0, 1])
        for at in range(0, lanes, LANES):
            block = slice(at, at + LANES)
            pace = jnp.dot(six_rows, pace_map[:, block], preferred_element_type=F32)
            surge = jnp.dot(six_rows, surge_map[:, block], preferred_element_type=F32)
            fall = rate[:, block] * pace
            size = jnp.exp(surge - fall)
            sin, cos = sin_cos(turn[:, block] * pace)
            by_re, by_im = size * cos, size * sin
            weight = jnp.sqrt(one_minus_exp(2.0 * fall))
            add_re = jnp.dot(ordered, in_re[:, block], preferred_element_type=F32) * weight
            add_im = jnp.dot(ordered, in_im[:, block], preferred_element_type=F32) * weight
            for k in range(steps):
                rows = slice(CHUNKS * k, CHUNKS * (k + 1))
                b_re, b_im, a_re, a_im = by_re[rows], by_im[rows], add_re[rows], add_im[rows]
                if k == 0:
                    p_re, p_im, s_re, s_im = b_re, b_im, a_re, a_im
                else:
                    p_re, p_im = b_re * p_re - b_im * p_im, b_re * p_im + b_im * p_re
                    s_re, s_im = b_re * s_re - b_im * s_im + a_re, b_re * s_im + b_im * s_re + a_im
                maps_ref[d, 0, rows, block] = p_re
                maps_ref[d, 1, rows, block] = p_im
                maps_ref[d, 2, rows, block] = s_re
                maps_ref[d, 3, rows, block] = s_im
            for i, part in enumerate((p_re, p_im, s_re, s_im)):
                tail_ref[i, :, block] = part
        total = [tail_ref[i, 0:1, :] for i in range(4)]
        for c in range(1, CHUNKS):
            p_re, p_im, s_re, s_im = (tail_ref[i, c : c + 1, :] for i in range(4))
            t_re, t_im, e_re, e_im = total
            total = [
                p_re * t_re - p_im * t_im,
                p_re * t_im + p_im * t_re,
                p_re * e_re - p_im * e_im + s_re,
                p_re * e_im + p_im * e_re + s_im,
            ]
        for i in range(4):
            ends_ref[4 * d + i : 4 * d + i + 1, :] = total[i]


def settle_kernel(
    place_ref, maps_ref, ends_ref, input_ref, skip_ref, gain_ref, long_maps_ref, short_maps_ref, merged_ref, carry_ref
):
    tokens, width = input_ref.shape
    lanes = maps_ref.shape[3]
    steps = tokens // CHUNKS
    members = ends_ref.shape[0]
    me = place_ref[1]
    total = jnp.zeros((tokens, width), F32)
    for d in range(2):
        c_re = jnp.zeros((1, lanes), F32)
        c_im = jnp.zeros((1, lanes), F32)
        order = range(members - 1, -1, -1) if d else range(members)
        for s in order:
            p_re, p_im, s_re, s_im = (ends_ref[s, 4 * d + i : 4 * d + i + 1, :] for i in range(4))
            reached = (s > me) if d else (s < me)
            n_re = p_re * c_re - p_im * c_im + s_re
            n_im = p_re * c_im + p_im * c_re + s_im
            c_re = jnp.where(reached, n_re, c_re)
            c_im = jnp.where(reached, n_im, c_im)
        last = CHUNKS * (steps - 1)
        for c in range(CHUNKS):
            carry_ref[0, c : c + 1, :] = c_re
            carry_ref[1, c : c + 1, :] = c_im
            p_re, p_im, s_re, s_im = (maps_ref[d, i, last + c : last + c + 1, :] for i in range(4))
            c_re, c_im = p_re * c_re - p_im * c_im + s_re, p_re * c_im + p_im * c_re + s_im
        out_re = spread(long_maps_ref[d, 1, 0], short_maps_ref[d, 1, 0])
        out_im = spread(long_maps_ref[d, 1, 1], short_maps_ref[d, 1, 1])
        read = jnp.zeros((tokens, width), F32)
        for at in range(0, lanes, LANES):
            block = slice(at, at + LANES)
            e_re = jnp.concatenate([carry_ref[0, :, block]] * steps, axis=0)
            e_im = jnp.concatenate([carry_ref[1, :, block]] * steps, axis=0)
            p_re, p_im = maps_ref[d, 0, :, block], maps_ref[d, 1, :, block]
            state_re = maps_ref[d, 2, :, block] + p_re * e_re - p_im * e_im
            state_im = maps_ref[d, 3, :, block] + p_re * e_im + p_im * e_re
            contract = (((1,), (1,)), ((), ()))
            read += lax.dot_general(
                state_re.astype(BF16), out_re[:, block], contract, preferred_element_type=F32
            )
            read -= lax.dot_general(
                state_im.astype(BF16), out_im[:, block], contract, preferred_element_type=F32
            )
        place = time_of_row(iota((tokens, tokens), 1), tokens, d == 1) == iota((tokens, tokens), 0)
        place = jnp.where(place, 1.0, 0.0).astype(BF16)
        high = read.astype(BF16)
        low = (read - high.astype(F32)).astype(BF16)
        total += jnp.dot(place, high, preferred_element_type=F32)
        total += jnp.dot(place, low, preferred_element_type=F32)
    active = jax.nn.gelu(total + skip_ref[...] * input_ref[...].astype(F32))
    for at in range(0, width, NORM_W):
        block = slice(at, at + NORM_W)
        part = active[:, block]
        part = part * lax.rsqrt(jnp.mean(part * part, axis=1, keepdims=True) + EPSILON)
        merged_ref[:, block] = (part * gain_ref[:, block]).astype(BF16)


def project_kernel(place_ref, merged_ref, residual_ref, emit_ref, gain_ref, normed_ref, own_ref):
    _, members, tokens, width = merged_ref.shape
    features = residual_ref.shape[3]
    depth = members * features
    projected = jnp.zeros((tokens, depth), F32)
    for t in range(members):
        projected += jnp.dot(
            merged_ref[0, t], emit_ref[t * width : (t + 1) * width, :], preferred_element_type=F32
        )
    middle = projected + jnp.concatenate(
        [residual_ref[0, t].astype(F32) for t in range(members)], axis=1
    )
    scale = lax.rsqrt(jnp.mean(middle * middle, axis=1, keepdims=True) + EPSILON)
    normed_ref[...] = (middle * scale * gain_ref[...]).astype(BF16)
    for t in range(members):

        @pl.when((place_ref[0] == t) & (place_ref[2] == pl.program_id(0)))
        def _(t=t):
            own_ref[...] = middle[:, t * features : (t + 1) * features]


def feed_kernel(normed_ref, raise_ref, lower_ref, out_ref):
    members, features = out_ref.shape[1], out_ref.shape[3]
    upward = jnp.dot(normed_ref[...], raise_ref[...], preferred_element_type=F32)
    hidden = jnp.square(jnp.maximum(upward, 0.0)).astype(BF16)
    parts = [
        jnp.dot(hidden, lower_ref[s], preferred_element_type=F32).astype(BF16)
        for s in range(lower_ref.shape[0])
    ]
    whole = jnp.concatenate(parts, axis=1) if len(parts) > 1 else parts[0]
    for t in range(members):
        out_ref[0, t] = whole[:, t * features : (t + 1) * features]


def exchange(x, axes):
    return lax.all_to_all(x, axes, split_axis=0, concat_axis=0, tiled=True)


def everywhere(x, axes, members):
    return exchange(jnp.broadcast_to(x[None], (members,) + x.shape), axes)


def params(**more):
    return pltpu.CompilerParams(vmem_limit_bytes=56 * 1024 * 1024, **more)


def on_device(
    residual_signal, lifted_signal, discrete_timestep, additional_log_fading, paired_fading, unpaired_fading,
    paired_twist, unpaired_twist, paired_latent_linears, unpaired_latent_linears, skip_coefficient,
    closing_norm_multiplier, emitted_linear, leading_norm_multiplier, raising_linear, lowering_linear,
):
    members = lax.axis_size("tp")
    inner = lax.axis_size("q")
    line = HALVES * inner
    rank = lax.axis_index("tp")
    my_q = lax.axis_index("q")
    me = lax.axis_index("zh") * inner + my_q
    place = jnp.stack([rank, me, my_q]).astype(jnp.int32)
    tokens, width = lifted_signal.shape
    groups = discrete_timestep.shape[0]
    pairs = groups // 2
    long_states, short_states = paired_fading.shape[2], unpaired_fading.shape[2]
    lanes = pairs * (long_states + short_states)
    depth_rows, hidden_columns = raising_linear.shape
    depth = depth_rows * line
    features = residual_signal.shape[1]
    share = hidden_columns // inner

    raise_parts = raising_linear.reshape(depth_rows, inner, share).transpose(1, 0, 2)
    raise_parts = jnp.concatenate([raise_parts] * HALVES, axis=0)
    lower_parts = lowering_linear.reshape(inner, share, depth_rows)
    lower_parts = jnp.concatenate([lower_parts] * HALVES, axis=0)
    raised = exchange(raise_parts, ("zh", "q")).reshape(depth, share)
    lowered = exchange(lower_parts, ("zh", "q"))
    if depth_rows % LANES:
        lowered = lowered.transpose(1, 0, 2).reshape(1, share, depth)
    residual_all = everywhere(residual_signal, ("q", "tp"), inner * members).reshape(
        inner, members, tokens, features
    )

    long_maps = jnp.swapaxes(paired_latent_linears, 4, 5)
    short_maps = jnp.swapaxes(unpaired_latent_linears, 4, 5)

    def owned(*shape, at):
        return pl.BlockSpec(shape, lambda i, place_ref: tuple(place_ref[0] if k == at else 0 for k in range(len(shape))))

    def rates(states):
        return pl.BlockSpec((2, None, pairs, states), lambda i, place_ref: (0, place_ref[0], 0, 0))

    def by_rank(array):
        return array.reshape(2, members, pairs, array.shape[2])

    def full(*shape):
        return pl.BlockSpec(shape, lambda i, place_ref: (0,) * len(shape))

    long_spec = owned(2, 2, 2, pairs, CHAN, long_states, at=3)
    short_spec = owned(2, 2, 2, pairs, CHAN, short_states, at=3)
    maps, ends = pl.pallas_call(
        scan_kernel,
        grid_spec=pltpu.PrefetchScalarGridSpec(
            num_scalar_prefetch=1,
            grid=(1,),
            in_specs=[
                full(tokens, width),
                full(groups, tokens),
                full(groups, tokens),
                rates(long_states),
                rates(short_states),
                rates(long_states),
                rates(short_states),
                long_spec,
                short_spec,
            ],
            out_specs=[full(2, 4, tokens, lanes), full(8, lanes)],
            scratch_shapes=[pltpu.VMEM((4, CHUNKS, lanes), F32)],
        ),
        out_shape=[
            jax.ShapeDtypeStruct((2, 4, tokens, lanes), F32),
            jax.ShapeDtypeStruct((8, lanes), F32),
        ],
        compiler_params=params(),
        name="scan",
    )(
        place, lifted_signal, discrete_timestep, additional_log_fading, by_rank(paired_fading),
        by_rank(unpaired_fading), by_rank(paired_twist), by_rank(unpaired_twist), long_maps, short_maps,
    )
    all_ends = everywhere(ends, ("zh", "q"), line)
    merged = pl.pallas_call(
        settle_kernel,
        grid_spec=pltpu.PrefetchScalarGridSpec(
            num_scalar_prefetch=1,
            grid=(1,),
            in_specs=[
                full(2, 4, tokens, lanes),
                full(line, 8, lanes),
                full(tokens, width),
                owned(1, width, at=1),
                owned(1, width, at=1),
                long_spec,
                short_spec,
            ],
            out_specs=full(tokens, width),
            scratch_shapes=[pltpu.VMEM((2, CHUNKS, lanes), F32)],
        ),
        out_shape=jax.ShapeDtypeStruct((tokens, width), BF16),
        compiler_params=params(),
        name="settle",
    )(
        place, maps, all_ends, lifted_signal, skip_coefficient[None], closing_norm_multiplier[None],
        long_maps, short_maps,
    )
    merged_all = everywhere(merged, ("q", "tp"), inner * members).reshape(inner, members, tokens, width)

    normed, own = pl.pallas_call(
        project_kernel,
        grid_spec=pltpu.PrefetchScalarGridSpec(
            num_scalar_prefetch=1,
            grid=(inner,),
            in_specs=[
                pl.BlockSpec((1, members, tokens, width), lambda i, place_ref: (i, 0, 0, 0)),
                pl.BlockSpec((1, members, tokens, features), lambda i, place_ref: (i, 0, 0, 0)),
                full(members * width, depth),
                full(1, depth),
            ],
            out_specs=[
                pl.BlockSpec((tokens, depth), lambda i, place_ref: (i, 0)),
                full(tokens, features),
            ],
        ),
        out_shape=[
            jax.ShapeDtypeStruct((inner * tokens, depth), BF16),
            jax.ShapeDtypeStruct((tokens, features), F32),
        ],
        compiler_params=params(),
        name="project",
    )(place, merged_all, residual_all, emitted_linear, leading_norm_multiplier[None])

    partial = pl.pallas_call(
        feed_kernel,
        grid=(inner,),
        in_specs=[
            pl.BlockSpec((tokens, depth), lambda i: (i, 0)),
            pl.BlockSpec((depth, share), lambda i: (0, 0)),
            pl.BlockSpec(lowered.shape, lambda i: (0, 0, 0)),
        ],
        out_specs=pl.BlockSpec((1, members, tokens, features), lambda i: (i, 0, 0, 0)),
        out_shape=jax.ShapeDtypeStruct((inner, members, tokens, features), BF16),
        compiler_params=params(),
        name="feed",
    )(normed, raised, lowered)
    shares = exchange(partial.reshape(inner * members, tokens, features), ("q", "tp"))
    return (own + jnp.sum(shares.astype(F32), axis=0)).astype(BF16)


def solution(mesh):
    sp, tp = mesh.axis_names
    line, members = mesh.shape[sp], mesh.shape[tp]
    split = Mesh(mesh.devices.reshape(HALVES, line // HALVES, members), ("zh", "q", "tp"))
    s, t = ("zh", "q"), "tp"
    in_specs = (P(s, t), P(s, t), P(t, s), P(t, s)) + (P(),) * 10 + (P(s, t), P(t, s))
    return jax.shard_map(
        on_device, mesh=split, in_specs=in_specs, out_specs=P(s, t), check_vma=False
    )
```

```python
import jax
import jax.numpy as jnp
from jax import lax
from jax.experimental import pallas as pl
from jax.experimental.pallas import tpu as pltpu
from jax.sharding import Mesh
from jax.sharding import PartitionSpec as P


CHAN = 16
NORM_W = 128
CHUNKS = 8
LANES = 128
EPSILON = 1e-06
HALVES = 2
SIN = (3.1415926532428884, -5.167712741152494, 2.5501627931734125, -0.5992473907509345, 0.08203117351788075, -0.00700041798679132)
COS = (0.9999999997799042, -4.934802137078826, 4.058709159556303, -1.33521200305024, 0.23493731381503577, -0.02439632434807213)
FADE = (1.0, -1.0 / 2, 1.0 / 6, -1.0 / 24, 1.0 / 120, -1.0 / 720, 1.0 / 5040, -1.0 / 40320)
CORES = 2
EVERY = ("zh", "q", "y", "c")
F32 = jnp.float32
BF16 = jnp.bfloat16


def horner(coefficients, x):
    total = jnp.full_like(x, coefficients[-1])
    for c in coefficients[-2::-1]:
        total = total * x + c
    return total


def sin_cos(angle):
    halves = angle * 0.3183098861837907
    whole = jnp.round(halves)
    r = halves - whole
    z = r * r
    odd = whole * 0.5
    odd = odd - jnp.floor(odd)
    sign = 1.0 - 4.0 * odd
    return sign * r * horner(SIN, z), sign * horner(COS, z)


def one_minus_exp(z):
    return jnp.where(z < 0.5, z * horner(FADE, z), 1.0 - jnp.exp(-z))


def iota(shape, axis):
    return lax.broadcasted_iota(jnp.int32, shape, axis)


def time_of_row(row, tokens, backward):
    steps = tokens // CHUNKS
    t = (row % CHUNKS) * steps + row // CHUNKS
    return tokens - 1 - t if backward else t


def group_of_lane(lane, pairs, long_states, short_states):
    border = pairs * long_states
    return jnp.where(
        lane < border,
        2 * (lane // long_states),
        2 * ((lane - border) // short_states) + 1,
    )


def tiled(part, copies):
    return jnp.concatenate([part] * copies, axis=-1) if copies > 1 else part


def spread(long_part, short_part):
    pairs, chan, long_states = long_part.shape
    short_states = short_part.shape[2]
    rows = pairs * 2 * chan
    long_rows = jnp.concatenate([long_part, jnp.zeros_like(long_part)], axis=1)
    short_rows = jnp.concatenate([jnp.zeros_like(short_part), short_part], axis=1)
    halves = []
    for part, states in ((long_rows, long_states), (short_rows, short_states)):
        part = part.reshape(rows, states)
        part = tiled(part, LANES // states)
        part = tiled(part, pairs * states // LANES)
        keep = iota(part.shape, 1) // states == iota(part.shape, 0) // (2 * chan)
        halves.append(jnp.where(keep, part, 0.0))
    return jnp.concatenate(halves, axis=1).astype(BF16)


def flat_row(long_part, short_part):
    halves = []
    for part in (long_part, short_part):
        pairs, states = part.shape
        wide = tiled(tiled(part, LANES // states), pairs * states // LANES)
        keep = iota(wide.shape, 1) // states == iota(wide.shape, 0)
        halves.append(jnp.sum(jnp.where(keep, wide, 0.0), axis=0, keepdims=True))
    return jnp.concatenate(halves, axis=1)


def three_parts(x):
    high = x.astype(BF16).astype(F32)
    rest = x - high
    middle = rest.astype(BF16).astype(F32)
    return [high, middle, rest - middle]


def scan_kernel(
    rank_ref, input_ref, pace_ref, surge_ref, long_rate_ref, short_rate_ref, long_turn_ref, short_turn_ref,
    long_maps_ref, short_maps_ref, maps_ref, ends_ref, tail_ref,
):
    tokens, _ = input_ref.shape
    groups = pace_ref.shape[0]
    _, pairs, long_states = long_rate_ref.shape
    short_states = short_rate_ref.shape[2]
    lanes = pairs * (long_states + short_states)
    steps = tokens // CHUNKS
    pieces = three_parts(pace_ref[...]) + three_parts(surge_ref[...])
    six = jnp.concatenate(pieces, axis=0).astype(BF16)
    inputs = input_ref[...]
    row = iota((6 * groups, lanes), 0)
    owner = group_of_lane(iota((6 * groups, lanes), 1), pairs, long_states, short_states)
    match = row % groups == owner
    pace_map = jnp.where(match & (row < 3 * groups), 1.0, 0.0).astype(BF16)
    surge_map = jnp.where(match & (row >= 3 * groups), 1.0, 0.0).astype(BF16)
    for d in range(2):
        place = time_of_row(iota((tokens, tokens), 0), tokens, d == 1) == iota((tokens, tokens), 1)
        place = jnp.where(place, 1.0, 0.0).astype(BF16)
        ordered = jnp.dot(place, inputs, preferred_element_type=F32).astype(BF16)
        six_rows = lax.dot_general(
            place, six, (((1,), (1,)), ((), ())), preferred_element_type=F32
        ).astype(BF16)
        rate = flat_row(long_rate_ref[d], short_rate_ref[d])
        turn = flat_row(long_turn_ref[d], short_turn_ref[d])
        in_re = spread(long_maps_ref[d, 0, 0], short_maps_ref[d, 0, 0])
        in_im = spread(long_maps_ref[d, 0, 1], short_maps_ref[d, 0, 1])
        for at in range(0, lanes, LANES):
            block = slice(at, at + LANES)
            pace = jnp.dot(six_rows, pace_map[:, block], preferred_element_type=F32)
            surge = jnp.dot(six_rows, surge_map[:, block], preferred_element_type=F32)
            fall = rate[:, block] * pace
            size = jnp.exp(surge - fall)
            sin, cos = sin_cos(turn[:, block] * pace)
            by_re, by_im = size * cos, size * sin
            weight = jnp.sqrt(one_minus_exp(2.0 * fall))
            add_re = jnp.dot(ordered, in_re[:, block], preferred_element_type=F32) * weight
            add_im = jnp.dot(ordered, in_im[:, block], preferred_element_type=F32) * weight
            for k in range(steps):
                rows = slice(CHUNKS * k, CHUNKS * (k + 1))
                b_re, b_im, a_re, a_im = by_re[rows], by_im[rows], add_re[rows], add_im[rows]
                if k == 0:
                    p_re, p_im, s_re, s_im = b_re, b_im, a_re, a_im
                else:
                    p_re, p_im = b_re * p_re - b_im * p_im, b_re * p_im + b_im * p_re
                    s_re, s_im = b_re * s_re - b_im * s_im + a_re, b_re * s_im + b_im * s_re + a_im
                maps_ref[d, 0, rows, block] = p_re
                maps_ref[d, 1, rows, block] = p_im
                maps_ref[d, 2, rows, block] = s_re
                maps_ref[d, 3, rows, block] = s_im
            for i, part in enumerate((p_re, p_im, s_re, s_im)):
                tail_ref[i, :, block] = part
        total = [tail_ref[i, 0:1, :] for i in range(4)]
        for c in range(1, CHUNKS):
            p_re, p_im, s_re, s_im = (tail_ref[i, c : c + 1, :] for i in range(4))
            t_re, t_im, e_re, e_im = total
            total = [
                p_re * t_re - p_im * t_im,
                p_re * t_im + p_im * t_re,
                p_re * e_re - p_im * e_im + s_re,
                p_re * e_im + p_im * e_re + s_im,
            ]
        for i in range(4):
            ends_ref[0, 4 * d + i : 4 * d + i + 1, :] = total[i]
    for s in range(1, ends_ref.shape[0]):
        ends_ref[s] = ends_ref[0]


def settle_kernel(
    place_ref, maps_ref, ends_ref, input_ref, skip_ref, gain_ref, long_maps_ref, short_maps_ref, residual_ref,
    rows_ref, carry_ref,
):
    tokens, width = input_ref.shape
    lanes = maps_ref.shape[3]
    steps = tokens // CHUNKS
    members = ends_ref.shape[0]
    rows = rows_ref.shape[1]
    me = place_ref[1]
    total = jnp.zeros((tokens, width), F32)
    for d in range(2):
        c_re = jnp.zeros((1, lanes), F32)
        c_im = jnp.zeros((1, lanes), F32)
        order = range(members - 1, -1, -1) if d else range(members)
        for s in order:
            p_re, p_im, s_re, s_im = (ends_ref[s, 4 * d + i : 4 * d + i + 1, :] for i in range(4))
            reached = (s > me) if d else (s < me)
            n_re = p_re * c_re - p_im * c_im + s_re
            n_im = p_re * c_im + p_im * c_re + s_im
            c_re = jnp.where(reached, n_re, c_re)
            c_im = jnp.where(reached, n_im, c_im)
        last = CHUNKS * (steps - 1)
        for c in range(CHUNKS):
            carry_ref[0, c : c + 1, :] = c_re
            carry_ref[1, c : c + 1, :] = c_im
            p_re, p_im, s_re, s_im = (maps_ref[d, i, last + c : last + c + 1, :] for i in range(4))
            c_re, c_im = p_re * c_re - p_im * c_im + s_re, p_re * c_im + p_im * c_re + s_im
        out_re = spread(long_maps_ref[d, 1, 0], short_maps_ref[d, 1, 0])
        out_im = spread(long_maps_ref[d, 1, 1], short_maps_ref[d, 1, 1])
        read = jnp.zeros((tokens, width), F32)
        for at in range(0, lanes, LANES):
            block = slice(at, at + LANES)
            e_re = jnp.concatenate([carry_ref[0, :, block]] * steps, axis=0)
            e_im = jnp.concatenate([carry_ref[1, :, block]] * steps, axis=0)
            p_re, p_im = maps_ref[d, 0, :, block], maps_ref[d, 1, :, block]
            state_re = maps_ref[d, 2, :, block] + p_re * e_re - p_im * e_im
            state_im = maps_ref[d, 3, :, block] + p_re * e_im + p_im * e_re
            contract = (((1,), (1,)), ((), ()))
            read += lax.dot_general(
                state_re.astype(BF16), out_re[:, block], contract, preferred_element_type=F32
            )
            read -= lax.dot_general(
                state_im.astype(BF16), out_im[:, block], contract, preferred_element_type=F32
            )
        place = time_of_row(iota((tokens, tokens), 1), tokens, d == 1) == iota((tokens, tokens), 0)
        place = jnp.where(place, 1.0, 0.0).astype(BF16)
        high = read.astype(BF16)
        low = (read - high.astype(F32)).astype(BF16)
        total += jnp.dot(place, high, preferred_element_type=F32)
        total += jnp.dot(place, low, preferred_element_type=F32)
    active = jax.nn.gelu(total + skip_ref[...] * input_ref[...].astype(F32))
    for at in range(0, width, NORM_W):
        block = slice(at, at + NORM_W)
        part = active[:, block]
        part = part * lax.rsqrt(jnp.mean(part * part, axis=1, keepdims=True) + EPSILON)
        part = (part * gain_ref[:, block]).astype(BF16)
        for t in range(rows_ref.shape[0]):
            rows_ref[t, :, block] = part[t * rows : (t + 1) * rows]
    for t in range(rows_ref.shape[0]):
        rows_ref[t, :, width:] = residual_ref[t * rows : (t + 1) * rows, :]


def project_kernel(rows_ref, emit_ref, gain_ref, normed_ref, middle_ref):
    members, features = middle_ref.shape[0], middle_ref.shape[2]
    width = rows_ref.shape[2] - features
    middle = jnp.concatenate([rows_ref[t, :, width:].astype(F32) for t in range(members)], axis=1)
    for t in range(members):
        middle += jnp.dot(
            rows_ref[t, :, :width], emit_ref[t * width : (t + 1) * width, :], preferred_element_type=F32
        )
    scale = lax.rsqrt(jnp.mean(middle * middle, axis=1, keepdims=True) + EPSILON)
    normed = (middle * scale * gain_ref[...]).astype(BF16)
    for t in range(members):
        middle_ref[t] = middle[:, t * features : (t + 1) * features]
    for i in range(normed_ref.shape[0]):
        for t in range(i % CORES, members, CORES):
            at = t // CORES * features
            normed_ref[i, :, at : at + features] = normed[:, t * features : (t + 1) * features]


def up_kernel(start_ref, normed_ref, *refs):
    *piece_refs, own_ref, sent_ref = refs
    blocks = len(piece_refs) // CORES
    deep, share = piece_refs[0].shape
    for j in range(CORES):
        total = 0.0
        for m in range(blocks):
            start = pl.multiple_of(start_ref[m], LANES) if blocks > 1 else 0
            total += jnp.dot(
                normed_ref[:, pl.ds(start, deep)], piece_refs[m * CORES + j][...], preferred_element_type=F32
            )
        own_ref[:, j * share : (j + 1) * share] = total
        sent_ref[:, j * share : (j + 1) * share] = total.astype(BF16)


def down_kernel(start_ref, own_ref, other_ref, *refs):
    *piece_refs, out_ref, total_ref = refs
    blocks = len(piece_refs) // CORES
    share, deep = piece_refs[0].shape
    parts, features = out_ref.shape[1], out_ref.shape[3]
    upward = own_ref[...] + other_ref[...].astype(F32)
    hidden = jnp.square(jnp.maximum(upward, 0.0)).astype(BF16)
    for m in range(blocks):
        start = pl.multiple_of(start_ref[m], LANES) if blocks > 1 else 0
        total_ref[:, pl.ds(start, deep)] = sum(
            jnp.dot(
                hidden[:, j * share : (j + 1) * share], piece_refs[m * CORES + j][...], preferred_element_type=F32
            )
            for j in range(CORES)
        )
    for y in range(parts):
        out_ref[0, y] = total_ref[:, y * features : (y + 1) * features].astype(BF16)


def without_bit(x, bit):
    return (x >> (bit + 1) << bit) | (x & ((1 << bit) - 1))


def with_bit(x, bit, value):
    return (x & ~(1 << bit)) | (value << bit)


def routes(line, rows_y):
    bit = (line // (rows_y * CORES)).bit_length() - 1
    found = {}
    for m in range(line):
        if m >> bit & 1:
            continue
        for j in range(CORES):
            pairs = []
            for s in range(line):
                for y in range(rows_y):
                    for c in range(CORES):
                        d = with_bit(s ^ m, bit, j ^ c)
                        pairs.append(((s * rows_y + y) * CORES + c, (d * rows_y + y) * CORES + (s >> bit & 1)))
            found[m, j] = pairs
    return bit, found


def exchange(x, axes):
    return lax.all_to_all(x, axes, split_axis=0, concat_axis=0, tiled=True)


def kernel(body, **more):
    return pl.pallas_call(body, **more)


def params(**more):
    return pltpu.CompilerParams(vmem_limit_bytes=56 * 1024 * 1024, **more)


def on_device(
    residual_signal, lifted_signal, discrete_timestep, additional_log_fading, paired_fading, unpaired_fading,
    paired_twist, unpaired_twist, paired_latent_linears, unpaired_latent_linears, skip_coefficient,
    closing_norm_multiplier, emitted_linear, leading_norm_multiplier, raising_linear, lowering_linear,
):
    rows_y = lax.axis_size("y")
    members = rows_y * CORES
    inner = lax.axis_size("q")
    line = HALVES * inner
    core = lax.axis_index("c")
    rank = lax.axis_index("y") * CORES + core
    me = lax.axis_index("zh") * inner + lax.axis_index("q")
    place = jnp.stack([rank, me]).astype(jnp.int32)
    tokens, width = lifted_signal.shape
    groups = discrete_timestep.shape[0]
    pairs = groups // 2
    long_states, short_states = paired_fading.shape[2], unpaired_fading.shape[2]
    lanes = pairs * (long_states + short_states)
    depth_rows, hidden_columns = raising_linear.shape
    depth = depth_rows * line
    half_depth = depth // CORES
    features = residual_signal.shape[1]
    share = hidden_columns // inner
    rows = tokens // members

    bit, found = routes(line, rows_y)
    up_pieces, down_pieces = [], []
    for (m, j), pairs_of in found.items():
        start = with_bit(me ^ m, bit, j ^ core) % inner * share
        up = lax.dynamic_slice_in_dim(raising_linear, start, share, 1)
        down = lax.dynamic_slice_in_dim(lowering_linear, start, share, 0)
        for piece, pieces in ((up, up_pieces), (down, down_pieces)):
            pieces.append(lax.ppermute(piece, EVERY, pairs_of))
    blocks = len(up_pieces) // CORES
    order = without_bit(me, bit) ^ jnp.arange(blocks)
    starts = (order * depth_rows).astype(jnp.int32)
    if depth_rows % LANES:
        up_pieces = [jnp.stack(up_pieces[j::CORES])[order].reshape(half_depth, share) for j in range(CORES)]
        down_pieces = [
            jnp.stack(down_pieces[j::CORES])[order].transpose(1, 0, 2).reshape(share, half_depth)
            for j in range(CORES)
        ]

    long_maps = jnp.swapaxes(paired_latent_linears, 4, 5)
    short_maps = jnp.swapaxes(unpaired_latent_linears, 4, 5)

    def owned(*shape, at):
        return pl.BlockSpec(shape, lambda i, place_ref: tuple(place_ref[0] if k == at else 0 for k in range(len(shape))))

    def rates(states):
        return pl.BlockSpec((2, None, pairs, states), lambda i, place_ref: (0, place_ref[0], 0, 0))

    def by_rank(array):
        return array.reshape(2, members, pairs, array.shape[2])

    def full(*shape):
        return pl.BlockSpec(shape, lambda i, place_ref: (0,) * len(shape))

    long_spec = owned(2, 2, 2, pairs, CHAN, long_states, at=3)
    short_spec = owned(2, 2, 2, pairs, CHAN, short_states, at=3)
    maps, ends = kernel(
        scan_kernel,
        grid_spec=pltpu.PrefetchScalarGridSpec(
            num_scalar_prefetch=1,
            grid=(1,),
            in_specs=[
                full(tokens, width),
                full(groups, tokens),
                full(groups, tokens),
                rates(long_states),
                rates(short_states),
                rates(long_states),
                rates(short_states),
                long_spec,
                short_spec,
            ],
            out_specs=[full(2, 4, tokens, lanes), full(line, 8, lanes)],
            scratch_shapes=[pltpu.VMEM((4, CHUNKS, lanes), F32)],
        ),
        out_shape=[
            jax.ShapeDtypeStruct((2, 4, tokens, lanes), F32),
            jax.ShapeDtypeStruct((line, 8, lanes), F32),
        ],
        compiler_params=params(),
    )(
        place, lifted_signal, discrete_timestep, additional_log_fading, by_rank(paired_fading),
        by_rank(unpaired_fading), by_rank(paired_twist), by_rank(unpaired_twist), long_maps, short_maps,
    )
    all_ends = exchange(ends, ("zh", "q"))
    mixed = kernel(
        settle_kernel,
        grid_spec=pltpu.PrefetchScalarGridSpec(
            num_scalar_prefetch=1,
            grid=(1,),
            in_specs=[
                full(2, 4, tokens, lanes),
                full(line, 8, lanes),
                full(tokens, width),
                owned(1, width, at=1),
                owned(1, width, at=1),
                long_spec,
                short_spec,
                full(tokens, features),
            ],
            out_specs=full(members, rows, width + features),
            scratch_shapes=[pltpu.VMEM((2, CHUNKS, lanes), F32)],
        ),
        out_shape=jax.ShapeDtypeStruct((members, rows, width + features), BF16),
        compiler_params=params(),
    )(
        place, maps, all_ends, lifted_signal, skip_coefficient[None], closing_norm_multiplier[None],
        long_maps, short_maps, residual_signal,
    )
    mixed_rows = exchange(mixed, ("y", "c"))
    normed, middle = kernel(
        project_kernel,
        out_shape=[
            jax.ShapeDtypeStruct((inner * members, rows, half_depth), BF16),
            jax.ShapeDtypeStruct((members, rows, features), F32),
        ],
        compiler_params=params(),
    )(mixed_rows, emitted_linear, leading_norm_multiplier[None])
    normed_all = exchange(normed, ("q", "y", "c")).reshape(inner * tokens, half_depth)
    middle_own = exchange(middle, ("y", "c")).reshape(tokens, features)

    def block(*shape):
        return pl.BlockSpec(shape, lambda i, start_ref: (i,) + (0,) * (len(shape) - 1))

    hidden_wide = CORES * share
    own, sent = kernel(
        up_kernel,
        grid_spec=pltpu.PrefetchScalarGridSpec(
            num_scalar_prefetch=1,
            grid=(inner,),
            in_specs=[block(tokens, half_depth)] + [full(*piece.shape) for piece in up_pieces],
            out_specs=[block(tokens, hidden_wide), block(tokens, hidden_wide)],
        ),
        out_shape=[
            jax.ShapeDtypeStruct((inner * tokens, hidden_wide), F32),
            jax.ShapeDtypeStruct((inner * tokens, hidden_wide), BF16),
        ],
        compiler_params=params(),
    )(starts, normed_all, *up_pieces)
    other = lax.ppermute(sent, "c", [(c, CORES - 1 - c) for c in range(CORES)])
    partial = kernel(
        down_kernel,
        grid_spec=pltpu.PrefetchScalarGridSpec(
            num_scalar_prefetch=1,
            grid=(inner,),
            in_specs=[block(tokens, hidden_wide), block(tokens, hidden_wide)]
            + [full(*piece.shape) for piece in down_pieces],
            out_specs=block(1, rows_y, tokens, features),
            scratch_shapes=[pltpu.VMEM((tokens, half_depth), F32)],
        ),
        out_shape=jax.ShapeDtypeStruct((inner, rows_y, tokens, features), BF16),
        compiler_params=params(),
    )(starts, own, other, *down_pieces)
    shares = exchange(partial.reshape(inner * rows_y, tokens, features), ("q", "y"))
    return (middle_own + jnp.sum(shares.astype(F32), axis=0)).astype(BF16)


def solution(mesh):
    sp, tp = mesh.axis_names
    line, members = mesh.shape[sp], mesh.shape[tp]
    rows_y = members // CORES
    split = Mesh(mesh.devices.reshape(HALVES, line // HALVES, rows_y, CORES), EVERY)
    s, t = EVERY[:2], EVERY[2:]
    in_specs = (P(s, t), P(s, t), P(t, s), P(t, s)) + (P(),) * 10 + (P(s, t), P(t, s))
    return jax.shard_map(
        on_device, mesh=split, in_specs=in_specs, out_specs=P(s, t), check_vma=False
    )
```
